32 devices in a mesh: ep: 4 (over y, x), tp: 8 (over z, core).
Axes of the slice: x: 2, y: 2, z: 4, core: 2. Of those that a mesh axis runs over, the one named last changes fastest.
Arguments:
- tokens: bfloat16 [64, 4096], P('ep'), may hold values from -6 to 6
- attn_gain: float32 [4096], replicated, may hold values from 0.1 to 1.9
- w_query: bfloat16 [4096, 2048], P('ep', 'tp'), may hold values from -0.15625 to 0.15625
- w_key: bfloat16 [4096, 2048], P('ep', 'tp'), may hold values from -0.09375 to 0.09375
- w_value: bfloat16 [4096, 2048], P('ep', 'tp'), may hold values from -0.09375 to 0.09375
- mix_lambda: float32 [16], P('tp'), may hold values from 0.3 to 0.8
- head_gain: float32 [128], replicated, may hold values from 0.1 to 1.9
- w_output: bfloat16 [2048, 4096], P('tp'), may hold values from -0.125 to 0.125
- cache_keys: bfloat16 [64, 1024, 2048], P('ep', None, 'tp'), may hold values from -180 to 180
- cache_value: bfloat16 [64, 1024, 2048], P('ep', None, 'tp'), may hold values from -6 to 6
- lengths: int32 [64], P('ep'), may hold values from 1 to 1024
- moe_gain: float32 [4096], replicated, may hold values from 0.1 to 1.9
- group_ids: int32 [64], P('ep'), may hold values from 0 to 1, as said below
- member_ids: int32 [64, 2], P('ep'), may hold values from 0 to 1, as said below
- group_gate: float32 [64], P('ep'), may hold values from 0.3 to 1
- member_logits: float32 [64, 2], P('ep'), may hold values from -4 to 4
- w_exp_gate: bfloat16 [4, 4096, 2048], P('ep', None, 'tp'), may hold values from -0.09375 to 0.09375
- w_exp_up: bfloat16 [4, 4096, 2048], P('ep', None, 'tp'), may hold values from -0.09375 to 0.09375
- w_exp_down: bfloat16 [4, 2048, 4096], P('ep', 'tp'), may hold values from -0.125 to 0.125
Outputs:
- mixed: bfloat16 [64, 4096], P('ep', 'tp')
- fresh_keys: bfloat16 [64, 2048], P('ep', 'tp')
- fresh_value: bfloat16 [64, 2048], P('ep', 'tp')
The draws below stay inside these ranges and needn't reach their ends.
Inputs may be any that keep to these rules, and one draw needn't show every extreme that they name: `group_ids`: each index of ep holds 16 consecutive tokens, of which every group gets the same number. A token's 2 members differ, and every expert group_ids * 2 + member_ids receives exactly 8 of the token-expert pairs of each index of ep.
All inputs are finite; a program needn't handle non-finite values.
Results may differ from the reference program's by a relative error of at most 0.015.
The reference program's roundings to bfloat16 on the way count: a program that leaves them out, or rounds other values in their place, can miss the bound.
Values may be sent and summed in bfloat16 or wider, within the bound.
No kernel may reach another device: no remote copies, remote signals or barrier semaphores. Data moves between devices by JAX's collectives and lax.ppermute only.
A program may use at most 64 MiB of HBM per device.

```python
import jax
import jax.numpy as jnp
from jax import lax

D = 4096
HEADS = 16
DH = 64
FF = 2048
EPG = 2
TOPK = 2
SEQ_DEV = 16
CACHE = 1024
EXPERTS = 4
GROUPS = 2
BATCH = 64
N_EP = 4
N_TP = 8


def routing_tables(key):
    perm_key, start_key, shift_key = jax.random.split(jax.random.fold_in(key, 11), 3)
    perms = jax.vmap(lambda sub: jax.random.permutation(sub, SEQ_DEV))(jax.random.split(perm_key, N_EP))
    starts = jax.random.randint(start_key, (N_EP, GROUPS), 0, EPG)
    shifts = jax.random.randint(shift_key, (N_EP, GROUPS), 1, EPG)
    group = perms % GROUPS
    inside = perms // GROUPS
    start_row = jnp.take_along_axis(starts, group, axis=1)
    shift_row = jnp.take_along_axis(shifts, group, axis=1)
    first = (start_row + inside) % EPG
    second = (start_row + inside + shift_row) % EPG
    members = jnp.stack([first, second], axis=-1)
    return (group.reshape(BATCH).astype(jnp.int32), members.reshape(BATCH, TOPK).astype(jnp.int32))


def draw_group_ids(key, part):
    group, members = routing_tables(key)
    return group


def draw_member_ids(key, part):
    group, members = routing_tables(key)
    return members


def draw_cache_keys(key, part):
    base_key = jax.random.fold_in(jax.random.fold_in(key, 21), 0)
    base = jax.random.truncated_normal(base_key, -6.0, 6.0, (BATCH, CACHE, HEADS * 2 * DH), jnp.float32)
    return base.astype(jnp.bfloat16)


def touch_ends(entries, key, least, top_value):
    place = [jax.random.randint(jax.random.fold_in(key, axis), (), 0, length) for axis, length in enumerate(entries.shape)]
    main_axis = entries.shape.index(max(entries.shape))
    next_to = place[:main_axis] + [(place[main_axis] + 1) % entries.shape[main_axis]] + place[main_axis + 1:]
    return entries.at[tuple(place)].set(least).at[tuple(next_to)].set(top_value)


def block_levels(key, dims, cuts, smallest, largest):
    loudness, own = 1.0, jax.random.fold_in(key, 6)
    for dim, blocks in cuts:
        draws = jnp.exp(jax.random.uniform(jax.random.fold_in(own, dim), (blocks,), jnp.float32, smallest / len(cuts), largest / len(cuts)))
        loudness = loudness * jnp.repeat(draws, dims[dim] // blocks).reshape([-1 if axis == dim else 1 for axis in range(len(dims))])
    return loudness


def gaussian(rng, dims, width, most, shards=(), held_as=jnp.bfloat16):
    level = block_levels(rng, dims, shards, -0.22, 0.18) if shards else 1.0
    values = jax.random.normal(rng, dims, jnp.float32) * width * level
    return jnp.minimum(jnp.maximum(values, -most), most).astype(held_as)


def setup_inputs(seed: int = 0) -> dict:
    key_of = jax.random.split(jax.random.key(seed), 20)
    return {
        "tokens": gaussian(key_of[0], (BATCH, D), 1.0, 6.0, ((0, 4),)),
        "attn_gain": jnp.clip(1.0 + 0.18 * jax.random.normal(key_of[1], (D,), jnp.float32), 0.1, 1.9),
        "w_query": gaussian(key_of[2], (D, HEADS * 2 * DH), (D // 3) ** -0.5, 0.15625, ((0, 4), (1, 8))),
        "w_key": gaussian(key_of[3], (D, HEADS * 2 * DH), D ** -0.5, 0.09375, ((0, 4), (1, 8))),
        "w_value": gaussian(key_of[4], (D, HEADS * 2 * DH), D ** -0.5, 0.09375, ((0, 4), (1, 8))),
        "mix_lambda": jnp.clip(0.3 + 0.5 * jax.random.uniform(key_of[5], (HEADS,), jnp.float32) ** block_levels(key_of[5], (HEADS,), ((0, 8),), -0.2, 0.2), 0.3, 0.8),
        "head_gain": jnp.clip(1.0 + 0.18 * jax.random.normal(key_of[6], (2 * DH,), jnp.float32), 0.1, 1.9),
        "w_output": gaussian(key_of[7], (HEADS * 2 * DH, D), (HEADS * 2 * DH) ** -0.5, 0.125, ((0, 8),)),
        "cache_keys": draw_cache_keys(jax.random.fold_in(key_of[19], 71), 0),
        "cache_value": gaussian(key_of[9], (BATCH, CACHE, HEADS * 2 * DH), 1.0, 6.0, ((0, 4), (2, 8))),
        "lengths": touch_ends(jax.random.randint(key_of[10], (BATCH,), 1, CACHE + 1), jax.random.fold_in(key_of[10], 1), 1, CACHE).astype(jnp.int32),
        "moe_gain": jnp.clip(1.0 + 0.18 * jax.random.normal(key_of[11], (D,), jnp.float32), 0.1, 1.9),
        "group_ids": draw_group_ids(jax.random.fold_in(key_of[19], 71), 0),
        "member_ids": draw_member_ids(jax.random.fold_in(key_of[19], 71), 0),
        "group_gate": jnp.clip(0.3 + 0.7 * jax.random.uniform(key_of[14], (BATCH,), jnp.float32) ** block_levels(key_of[14], (BATCH,), ((0, 4),), -0.2, 0.2), 0.3, 1.0),
        "member_logits": gaussian(key_of[15], (BATCH, TOPK), 1.0, 4.0, ((0, 4),), jnp.float32),
        "w_exp_gate": gaussian(key_of[16], (EXPERTS, D, FF), D ** -0.5, 0.09375, ((0, 4), (2, 8))),
        "w_exp_up": gaussian(key_of[17], (EXPERTS, D, FF), D ** -0.5, 0.09375, ((0, 4), (2, 8))),
        "w_exp_down": gaussian(key_of[18], (EXPERTS, FF, D), FF ** -0.5, 0.125, ((0, 4), (1, 8))),
    }


EPS = 1e-06

def rms_scale(values, gain):
    return values * lax.rsqrt(lax.optimization_barrier(jnp.mean(values * values, axis=-1, keepdims=True)) + EPS) * gain

def reference(tokens, attn_gain, w_query, w_key, w_value, mix_lambda, head_gain, w_output, cache_keys, cache_value, lengths, moe_gain, group_ids, member_ids, group_gate, member_logits, w_exp_gate, w_exp_up, w_exp_down):
    resid_in = tokens.astype(jnp.float32)
    normed = rms_scale(resid_in, attn_gain).astype(jnp.bfloat16)

    def project(weight):
        return jnp.dot(normed, weight, preferred_element_type=jnp.float32).astype(jnp.bfloat16)
    query = project(w_query)
    fresh_keys = project(w_key)
    fresh_val = project(w_value)
    head_index = jnp.arange(HEADS).astype(jnp.float32)
    slopes = 2.0 ** (-8.0 * (head_index + 1.0) / HEADS)
    scale = DH ** (-0.5)
    lam = mix_lambda.astype(jnp.float32)

    def block(args):
        qry, knew, vnew, ckeys, cval, lens = args
        count = qry.shape[0]
        positions = jnp.arange(CACHE)
        dist = (lens[:, None] - positions[None, :]).astype(jnp.float32)
        valid = positions[None, :] < lens[:, None]
        qf = qry.reshape(count, HEADS, 2, DH).astype(jnp.float32)
        keys = ckeys.reshape(count, CACHE, HEADS, 2, DH).astype(jnp.float32)
        fresh = knew.reshape(count, HEADS, 2, DH).astype(jnp.float32)
        old = jnp.einsum('shcd,slhcd->cshl', qf, keys, precision=lax.Precision.HIGHEST) * scale
        old = old - slopes[None, None, :, None] * dist[None, :, None, :]
        old = jnp.where(valid[None, :, None, :], old, -jnp.inf)
        new = jnp.moveaxis(lax.optimization_barrier(jnp.sum(qf * fresh, axis=-1)) * scale, 2, 0)
        full = jnp.concatenate([old, new[..., None]], axis=-1)
        maps = jax.nn.softmax(full, axis=-1)
        weights = (maps[0] - lam[None, :, None] * maps[1]).astype(jnp.bfloat16)
        values = cval.reshape(count, CACHE, HEADS, 2 * DH).astype(jnp.float32)
        wide = weights.astype(jnp.float32)
        head_mix = jnp.einsum('shl,slhe->she', wide[..., :CACHE], values, precision=lax.Precision.HIGHEST)
        head_mix = head_mix + wide[..., CACHE][..., None] * vnew.reshape(count, HEADS, 2 * DH).astype(jnp.float32)
        head_out = rms_scale(head_mix, head_gain).astype(jnp.bfloat16)
        return head_out.reshape(count, HEADS * 2 * DH)

    def split(array):
        return array.reshape((N_EP, SEQ_DEV) + array.shape[1:])
    pieces = (split(query), split(fresh_keys), split(fresh_val), split(cache_keys), split(cache_value), split(lengths))
    head_out = lax.map(block, pieces).reshape(BATCH, HEADS * 2 * DH)
    group = HEADS * 2 * DH // N_TP
    attn_sum = jnp.zeros((BATCH, D), jnp.float32)
    for index in range(N_TP):
        term = jnp.dot(head_out[:, index * group:(index + 1) * group], w_output[index * group:(index + 1) * group], preferred_element_type=jnp.float32).astype(jnp.bfloat16)
        attn_sum = attn_sum + lax.optimization_barrier(term).astype(jnp.float32)
    resid = resid_in + attn_sum
    moe_in = rms_scale(resid, moe_gain).astype(jnp.bfloat16)
    expert_ids = group_ids[:, None] * EPG + member_ids
    route_weight = jax.nn.softmax(member_logits.astype(jnp.float32), axis=-1) * group_gate[:, None]

    def step(total, args):
        gate_w, up_w, down_w, index = args
        gate = jnp.dot(moe_in, gate_w, preferred_element_type=jnp.float32)
        upper = jnp.dot(moe_in, up_w, preferred_element_type=jnp.float32)
        hidden = (jax.nn.silu(gate) * upper).astype(jnp.bfloat16)
        result = jnp.dot(hidden, down_w, preferred_element_type=jnp.float32).astype(jnp.bfloat16)
        share = lax.optimization_barrier(jnp.sum(jnp.where(expert_ids == index, route_weight, 0.0), axis=1))
        return (total + share[:, None] * lax.optimization_barrier(result).astype(jnp.float32), None)
    routed, _ = lax.scan(step, jnp.zeros((BATCH, D), jnp.float32), (w_exp_gate, w_exp_up, w_exp_down, jnp.arange(EXPERTS).astype(jnp.int32)))
    mixed = (resid + routed).astype(jnp.bfloat16)
    return (mixed, fresh_keys, fresh_val)
```

```python
import functools
import itertools

import jax
import jax.numpy as jnp
from jax import lax
from jax.experimental import pallas as pl
from jax.experimental.pallas import tpu as pltpu
from jax.sharding import PartitionSpec as P

EPG = 2
EPS = 1e-06
F32, BF16 = jnp.float32, jnp.bfloat16
LANES, SUB = 128, 8
CORES = 2
VMEM = pl.BlockSpec(memory_space=pltpu.VMEM)
HBM = pl.BlockSpec(memory_space=pltpu.HBM)
ANY = pl.BlockSpec(memory_space=pl.ANY)


def params(mib):
    return pltpu.CompilerParams(vmem_limit_bytes=mib << 20)


def cost(flops):
    return pl.CostEstimate(flops=int(flops), bytes_accessed=1 << 20, transcendentals=0)


def dot(a, b):
    return jnp.dot(a, b, preferred_element_type=F32)


def slabs(width, n_tp, parity):
    slab = width // n_tp
    for z in range(n_tp // CORES):
        start = (z * CORES + parity) * slab
        yield z, slice(z * slab, (z + 1) * slab), pl.ds(pl.multiple_of(start, LANES), slab)


def slices_kernel(tokens_hbm, gain_hbm, *refs):
    *outs, tokens, gain, sems = refs
    n = len(outs)
    seqs, width = tokens.shape
    cols = width // n
    copies = [pltpu.make_async_copy(gain_hbm, gain, sems.at[n])]
    for k in range(n):
        at = slice(k * cols, (k + 1) * cols)
        copies.append(pltpu.make_async_copy(tokens_hbm.at[:, at], tokens.at[:, at], sems.at[k]))
    for copy in copies:
        copy.start()
    for copy in copies:
        copy.wait()
    x = tokens[...].astype(F32)
    scale = lax.rsqrt(jnp.sum(x * x, axis=1, keepdims=True) * (1.0 / width) + EPS)
    for k, out in enumerate(outs):
        at = pl.ds(pl.multiple_of((lax.axis_index("ep") ^ k) * cols, LANES), cols)
        out[...] = (tokens[:, at].astype(F32) * scale * gain[:, at]).astype(BF16)


def tables_kernel(groups, group_ids, member_ids, logits, gate, picker, picks, shares):
    top, seqs = member_ids.shape
    cap = seqs // groups
    row = lax.broadcasted_iota(jnp.int32, (seqs, seqs), 0)
    col = lax.broadcasted_iota(jnp.int32, (seqs, seqs), 1)

    def column(line):
        return jnp.sum(jnp.where(row == col, line, 0.0), axis=1, keepdims=True)

    group = group_ids[...].astype(F32)
    same = column(group) == group
    rank_line = jnp.sum(jnp.where(same & (row < col), 1.0, 0.0), axis=0, keepdims=True)
    rank = jnp.sum(jnp.where(same & (col < row), 1.0, 0.0), axis=1, keepdims=True)
    spot = lax.broadcasted_iota(jnp.int32, picker.shape, 0)
    wanted = ((lax.axis_index("ep") ^ (spot // cap)) // EPG).astype(F32)
    here = (group == wanted) & (rank_line == (spot % cap).astype(F32))
    picker[...] = here.astype(F32).astype(BF16)
    route = jnp.exp(logits[...] - jnp.max(logits[...], axis=0, keepdims=True))
    route = route / jnp.sum(route, axis=0, keepdims=True) * gate[...]
    spot = lax.broadcasted_iota(jnp.int32, (seqs, picks.shape[1]), 1).astype(F32)
    for k in range(top):
        expert = column(group * EPG + member_ids[k : k + 1, :].astype(F32))
        picks[k * seqs : (k + 1) * seqs, :] = (expert * cap + rank == spot).astype(F32).astype(BF16)
        shares[k * seqs : (k + 1) * seqs, :] = jnp.broadcast_to(column(route[k : k + 1]), (seqs, LANES))


def project_kernel(n, *refs):
    ins, weights, outs = refs[:n], refs[n : n + 3], refs[n + 4 :]
    seqs = ins[0].shape[0]
    rows = jnp.concatenate([ref[...] for ref in ins], axis=0)
    for j, weight in enumerate(weights):
        cols = weight.shape[1]
        got = dot(rows, weight[...])
        for k, out in enumerate(outs):
            out[:, j * cols : (j + 1) * cols] = got[k * seqs : (k + 1) * seqs]


def attention_kernel(n, total_heads, lengths, lam, *refs):
    parts = refs[:n]
    head_gain, keys, values, w_out, mine, theirs, fresh_k, fresh_v, spread, scores, fresh_share, *mixed = refs[n:]
    seqs, spots, cols = keys.shape
    width = w_out.shape[1]
    heads = lam.shape[1]
    wide = cols // heads
    head_dim = wide // 2
    maps = 2 * heads
    used = maps * seqs
    per = SUB // maps
    total = parts[0][...]
    for part in parts[1:]:
        total = total + part[...]
    projected = total.astype(BF16)
    query, fresh, value = (projected[:, j * cols : (j + 1) * cols] for j in range(3))
    fresh_k[...] = fresh
    fresh_v[...] = value
    repeat = lax.broadcasted_iota(jnp.int32, (used, seqs), 0) // maps
    repeat = (repeat == lax.broadcasted_iota(jnp.int32, (used, seqs), 1)).astype(F32).astype(BF16)
    row = lax.broadcasted_iota(jnp.int32, (used, cols), 0)
    col = lax.broadcasted_iota(jnp.int32, (used, cols), 1)
    query = jnp.where(row % maps == col // head_dim, dot(repeat, query), 0.0)
    spread[...] = query
    factor = head_dim ** (-0.5)
    new = jnp.sum(query * dot(repeat, fresh), axis=1, keepdims=True) * factor
    inside = lax.broadcasted_iota(jnp.int32, (SUB, 1), 0) // maps

    def one_score(i, carry):
        at = pl.ds(pl.multiple_of(i * SUB, SUB), SUB)
        block, got = spread[at, :], 0.0
        for p in range(per):
            lhs = jnp.where(inside == p, block, 0.0).astype(BF16)
            got += lax.dot_general(lhs, keys[i * per + p], (((1,), (1,)), ((), ())), preferred_element_type=F32)
        scores[at, :] = got
        return carry

    lax.fori_loop(0, used // SUB, one_score, 0, unroll=True)
    line = lax.broadcasted_iota(jnp.int32, (used, LANES), 0)
    whose = line[:, :seqs] // maps == lax.broadcasted_iota(jnp.int32, (used, seqs), 1)
    count = jnp.sum(jnp.where(whose, lengths[...].astype(F32), 0.0), axis=1, keepdims=True)
    head = (lax.axis_index("tp") * heads + (line % maps) // 2).astype(F32)
    slope = jnp.exp2(-8.0 * (head + 1.0) / total_heads)
    mix = jnp.zeros((used, LANES), F32)
    for h in range(heads):
        mix = jnp.where((line % maps) // 2 == h, lam[:, h : h + 1], mix)
    pieces = []
    top = jnp.broadcast_to(new, (used, LANES))
    for at in range(0, spots, LANES):
        spot = (lax.broadcasted_iota(jnp.int32, (used, LANES), 1) + at).astype(F32)
        piece = scores[:, at : at + LANES] * factor - slope * (count - spot)
        piece = jnp.where(spot < count, piece, -jnp.inf)
        pieces.append(piece)
        top = jnp.maximum(top, piece)
    top = jnp.max(top, axis=1, keepdims=True)
    new = jnp.exp(new - top)
    pieces = [jnp.exp(piece - top) for piece in pieces]
    norm = 1.0 / (jnp.sum(functools.reduce(jnp.add, pieces), axis=1, keepdims=True) + new)

    def blend(piece):
        piece = piece * norm
        return piece - mix * pltpu.roll(piece, used - 1, 0)

    for j, piece in enumerate(pieces):
        scores[:, j * LANES : (j + 1) * LANES] = blend(piece)
    fresh_share[...] = blend(jnp.broadcast_to(new, (used, LANES)))

    def one_mix(i, carry):
        at = pl.ds(pl.multiple_of(i * SUB, SUB), SUB)
        block, got = scores[at, :], 0.0
        for p in range(per):
            lhs = jnp.where(inside == p, block, 0.0).astype(BF16)
            got += dot(lhs, values[i * per + p])
        for h in range(heads):
            mixed[h][at, :] = got[:, h * wide : (h + 1) * wide]
        return carry

    lax.fori_loop(0, used // SUB, one_mix, 0, unroll=True)
    outs = []
    for h in range(heads):
        at = slice(h * wide, (h + 1) * wide)
        rows = pl.ds(2 * h, seqs, stride=maps)
        share = fresh_share[rows, :].astype(BF16).astype(F32)
        both = mixed[h][rows, :] + share * value[:, at].astype(F32)
        mean = jnp.mean(both * both, axis=1, keepdims=True)
        outs.append((both * lax.rsqrt(mean + EPS) * head_gain[...]).astype(BF16))
    out = jnp.concatenate(outs, axis=1)
    first = lax.axis_index("tp") % CORES == 0
    slab = width * heads // total_heads
    for z in range(mine.shape[1] // slab):
        at, start = slice(z * slab, (z + 1) * slab), z * CORES * slab
        even, odd = (dot(out, w_out[:, lo : lo + slab]) for lo in (start, start + slab))
        mine[:, at] = jnp.where(first, even, odd).astype(BF16)
        theirs[:, at] = jnp.where(first, odd, even).astype(BF16)


def pair_kernel(mine, got, out):
    out[...] = (mine[...].astype(F32) + got[...].astype(F32)).astype(BF16)


def dispatch_kernel(n_ep, n_tp, n, picker, tokens, *refs):
    parts, resid, outs = refs[:n], refs[n], refs[n + 1 :]
    cap = outs[0].shape[0]
    index = lax.axis_index("tp")
    own = jnp.zeros(resid.shape, F32)
    for z, at, cut in slabs(tokens.shape[1], n_tp, index % CORES):
        total = parts[0][:, at].astype(F32)
        for part in parts[1:]:
            total = total + part[:, at].astype(F32)
        total = tokens[:, cut].astype(F32) + total
        own = jnp.where(index // CORES == z, total, own)
        rows = dot(picker[...], total.astype(BF16)).astype(BF16)
        for k, out in enumerate(outs):
            out[:, at] = rows[k * cap : (k + 1) * cap]
    resid[...] = own


def stack_kernel(*refs):
    for k, ref in enumerate(refs[:-1]):
        cap = ref.shape[0]
        refs[-1][k * cap : (k + 1) * cap, :] = ref[...]


def expert_kernel(n_ep, n_tp, mine, theirs, gain, w_gate, w_up, w_down, back):
    slab = back.shape[2]
    cap = back.shape[1] // n_tp
    width = slab * n_tp
    core = lax.axis_index("tp") % CORES
    blocks = []
    for head, tail, parity in ((mine, theirs, core), (theirs, mine, 1 - core)):
        for _, at, cut in slabs(width, n_tp, parity):
            blocks.append((cut, jnp.concatenate([head[:cap, at].astype(F32), tail[cap:, at].astype(F32)], axis=0)))
    square = sum(jnp.sum(x * x, axis=1, keepdims=True) for _, x in blocks)
    scale = lax.rsqrt(square * (1.0 / width) + EPS)
    gate, upper = 0.0, 0.0
    for cut, x in blocks:
        x = (x * scale * gain[:, cut]).astype(BF16)
        gate += dot(x, w_gate[0, cut, :])
        upper += dot(x, w_up[0, cut, :])
    hidden = (gate * (1.0 / (1.0 + jnp.exp(-gate))) * upper).astype(BF16)
    for t in range(n_tp):
        down = dot(hidden, w_down[0, :, t * slab : (t + 1) * slab]).astype(BF16)
        for k in range(n_ep):
            back[lax.axis_index("ep") ^ k, t * cap : (t + 1) * cap, :] = down[k * cap : (k + 1) * cap]


def combine_kernel(n_ep, n_tp, back, resid, picks, shares, mixed):
    seqs, slab = resid.shape
    cap = back.shape[0] // (n_ep * n_tp)
    outs = []
    for e in range(n_ep):
        total = jnp.zeros((cap, slab), F32)
        for t in range(n_tp):
            lo = (e * n_tp + t) * cap
            total = total + back[lo : lo + cap, :].astype(F32)
        outs.append(total)
    picked = dot(picks[...], jnp.concatenate(outs, axis=0).astype(BF16))
    total = resid[...]
    for k in range(picked.shape[0] // seqs):
        lines = slice(k * seqs, (k + 1) * seqs)
        total = total + shares[lines, :1] * picked[lines]
    mixed[...] = total.astype(BF16)


def on_device(
    n_ep, n_tp,
    tokens, attn_gain, w_query, w_key, w_value, mix_lambda, head_gain, w_output, cache_keys, cache_value, lengths,
    moe_gain, group_ids, member_ids, group_gate, member_logits, w_exp_gate, w_exp_up, w_exp_down,
):
    seqs, width = tokens.shape
    cols = w_query.shape[1]
    slab = width // n_tp
    groups = n_ep * w_exp_gate.shape[0] // EPG
    heads = mix_lambda.shape[0]
    shape = jax.ShapeDtypeStruct

    def send(piece, axis, count, k):
        return lax.ppermute(piece, axis, [(i, i ^ k) for i in range(count)])

    def swap(pieces):
        return [pieces[0]] + [send(piece, "ep", n_ep, k) for k, piece in enumerate(pieces) if k]

    def cross(pieces):
        pairs = itertools.product(range(n_ep), range(n_tp))
        pairs = [(e, t, e * n_tp + t) for e, t in pairs]
        return [pieces[0]] + [
            lax.ppermute(piece, ("ep", "tp"), [(i, (e ^ k) * n_tp + (t ^ 1)) for e, t, i in pairs])
            for k, piece in enumerate(pieces)
            if k
        ]

    slices = pl.pallas_call(
        slices_kernel,
        out_shape=[shape((seqs, width // n_ep), BF16)] * n_ep,
        in_specs=[HBM] * 2,
        out_specs=[VMEM] * n_ep,
        scratch_shapes=[
            pltpu.VMEM((seqs, width), BF16),
            pltpu.VMEM((1, width), F32),
            pltpu.SemaphoreType.DMA((n_ep + 1,)),
        ],
        compiler_params=params(2),
        cost_estimate=cost(2e10),
        name="slices",
    )(*(pltpu.with_memory_space_constraint(x, pltpu.HBM) for x in (tokens, attn_gain.reshape(1, width))))
    pairs = n_ep * n_tp * (seqs // groups)
    top = member_ids.shape[1]
    picker, picks, shares = pl.pallas_call(
        functools.partial(tables_kernel, groups),
        out_shape=[shape((pairs // n_tp, seqs), BF16), shape((top * seqs, pairs // n_tp), BF16), shape((top * seqs, LANES), F32)],
        in_specs=[VMEM] * 4,
        out_specs=[VMEM] * 3,
        compiler_params=params(2),
        cost_estimate=cost(1e9),
        name="tables",
    )(group_ids.reshape(1, seqs), member_ids.T, member_logits.T, group_gate.reshape(1, seqs))
    parts = pl.pallas_call(
        functools.partial(project_kernel, n_ep),
        out_shape=[shape((seqs, 3 * cols), F32)] * n_ep,
        in_specs=[VMEM] * (n_ep + 3) + [ANY],
        out_specs=[VMEM] * n_ep,
        compiler_params=params(6),
        cost_estimate=cost(2e10),
        name="project",
    )(*cross(slices), w_query, w_key, w_value, shares)
    mine, theirs, fresh_keys, fresh_value = pl.pallas_call(
        functools.partial(attention_kernel, n_ep, heads * n_tp),
        out_shape=[shape((seqs, width // CORES), BF16)] * 2 + [shape((seqs, cols), BF16)] * 2,
        in_specs=[VMEM] * (n_ep + 6),
        out_specs=[VMEM] * 4,
        scratch_shapes=[
            pltpu.VMEM((2 * heads * seqs, cols), F32),
            pltpu.VMEM((2 * heads * seqs, cache_keys.shape[1]), F32),
        ]
        + [pltpu.VMEM((2 * heads * seqs, LANES), F32)] * (1 + heads),
        compiler_params=params(6),
        cost_estimate=cost(1e10),
        name="attention",
    )(
        lengths.reshape(1, seqs), mix_lambda.reshape(1, heads), *swap(parts), head_gain.reshape(1, -1),
        cache_keys, cache_value, w_output,
    )
    pair = pl.pallas_call(
        pair_kernel,
        out_shape=shape(mine.shape, BF16),
        in_specs=[VMEM] * 2,
        out_specs=VMEM,
        compiler_params=params(2),
        cost_estimate=cost(5e8),
        name="pair",
    )(mine, send(theirs, "tp", n_tp, 1))
    halves = [pair] + [send(pair, "tp", n_tp, CORES * k) for k in range(1, n_tp // CORES)]
    cap = seqs // groups
    resid, *rows = pl.pallas_call(
        functools.partial(dispatch_kernel, n_ep, n_tp, len(halves)),
        out_shape=[shape((seqs, slab), F32)] + [shape((cap, width // CORES), BF16)] * n_ep,
        in_specs=[VMEM] * (2 + len(halves)),
        out_specs=[VMEM] * (1 + n_ep),
        compiler_params=params(2),
        cost_estimate=cost(5e9),
        name="dispatch",
    )(picker, tokens, *halves)
    mine = pl.pallas_call(
        stack_kernel,
        out_shape=shape((n_ep * cap, width // CORES), BF16),
        in_specs=[VMEM] * n_ep,
        out_specs=VMEM,
        compiler_params=params(2),
        cost_estimate=cost(5e8),
        name="stack",
    )(*cross(rows))
    back = pl.pallas_call(
        functools.partial(expert_kernel, n_ep, n_tp),
        out_shape=shape((n_ep, n_tp * cap, slab), BF16),
        in_specs=[VMEM] * 6,
        out_specs=VMEM,
        compiler_params=params(10),
        cost_estimate=cost(5e9),
        name="experts",
    )(mine, send(mine, "tp", n_tp, 1), moe_gain.reshape(1, width), w_exp_gate, w_exp_up, w_exp_down)
    back = back.reshape(pairs, slab)
    back = lax.all_to_all(back, ("ep", "tp"), split_axis=0, concat_axis=0, tiled=True)
    mixed = pl.pallas_call(
        functools.partial(combine_kernel, n_ep, n_tp),
        out_shape=shape((seqs, slab), BF16),
        in_specs=[VMEM] * 4,
        out_specs=VMEM,
        compiler_params=params(2),
        cost_estimate=cost(1e9),
        name="combine",
    )(back, resid, picks, shares)
    return mixed, fresh_keys, fresh_value


def solution(mesh):
    return jax.shard_map(
        functools.partial(on_device, mesh.shape["ep"], mesh.shape["tp"]),
        mesh=mesh,
        in_specs=(
            P("ep", None), P(), P("ep", "tp"), P("ep", "tp"), P("ep", "tp"), P("tp"), P(), P("tp", None),
            P("ep", None, "tp"), P("ep", None, "tp"), P("ep"), P(), P("ep"), P("ep", None), P("ep"), P("ep", None),
            P("ep", None, "tp"), P("ep", None, "tp"), P("ep", "tp", None),
        ),
        out_specs=(P("ep", "tp"), P("ep", "tp"), P("ep", "tp")),
        check_vma=False,
    )
```

```python
import functools
import itertools

import jax
import jax.numpy as jnp
from jax import lax
from jax.experimental import pallas as pl
from jax.experimental.pallas import tpu as pltpu
from jax.sharding import PartitionSpec as P

EPG = 2
EPS = 1e-06
F32, BF16 = jnp.float32, jnp.bfloat16
LANES, SUB = 128, 8
CORES = 2
VMEM = pl.BlockSpec(memory_space=pltpu.VMEM)
HBM = pl.BlockSpec(memory_space=pltpu.HBM)
ANY = pl.BlockSpec(memory_space=pl.ANY)


def params(mib):
    return pltpu.CompilerParams(vmem_limit_bytes=mib << 20)


def cost(flops):
    return pl.CostEstimate(flops=int(flops), bytes_accessed=1 << 20, transcendentals=0)


def dot(a, b):
    return jnp.dot(a, b, preferred_element_type=F32)


def slabs(width, n_tp, parity):
    slab = width // n_tp
    for z in range(n_tp // CORES):
        start = (z * CORES + parity) * slab
        yield z, slice(z * slab, (z + 1) * slab), pl.ds(pl.multiple_of(start, LANES), slab)


def slices_kernel(tokens_hbm, gain_hbm, *refs):
    *outs, tokens, gain, sems = refs
    n = len(outs)
    seqs, width = tokens.shape
    cols = width // n
    copies = [pltpu.make_async_copy(gain_hbm, gain, sems.at[n])]
    for k in range(n):
        at = slice(k * cols, (k + 1) * cols)
        copies.append(pltpu.make_async_copy(tokens_hbm.at[:, at], tokens.at[:, at], sems.at[k]))
    for copy in copies:
        copy.start()
    for copy in copies:
        copy.wait()
    x = tokens[...].astype(F32)
    scale = lax.rsqrt(jnp.sum(x * x, axis=1, keepdims=True) * (1.0 / width) + EPS)
    for k, out in enumerate(outs):
        at = pl.ds(pl.multiple_of((lax.axis_index("ep") ^ k) * cols, LANES), cols)
        out[...] = (tokens[:, at].astype(F32) * scale * gain[:, at]).astype(BF16)


def tables_kernel(groups, group_ids, member_ids, logits, gate, picker, picks, shares):
    top, seqs = member_ids.shape
    cap = seqs // groups
    row = lax.broadcasted_iota(jnp.int32, (seqs, seqs), 0)
    col = lax.broadcasted_iota(jnp.int32, (seqs, seqs), 1)

    def column(line):
        return jnp.sum(jnp.where(row == col, line, 0.0), axis=1, keepdims=True)

    group = group_ids[...].astype(F32)
    same = column(group) == group
    rank_line = jnp.sum(jnp.where(same & (row < col), 1.0, 0.0), axis=0, keepdims=True)
    rank = jnp.sum(jnp.where(same & (col < row), 1.0, 0.0), axis=1, keepdims=True)
    spot = lax.broadcasted_iota(jnp.int32, picker.shape, 0)
    wanted = ((lax.axis_index("ep") ^ (spot // cap)) // EPG).astype(F32)
    here = (group == wanted) & (rank_line == (spot % cap).astype(F32))
    picker[...] = here.astype(F32).astype(BF16)
    route = jnp.exp(logits[...] - jnp.max(logits[...], axis=0, keepdims=True))
    route = route / jnp.sum(route, axis=0, keepdims=True) * gate[...]
    spot = lax.broadcasted_iota(jnp.int32, (seqs, picks.shape[1]), 1).astype(F32)
    for k in range(top):
        expert = column(group * EPG + member_ids[k : k + 1, :].astype(F32))
        picks[k * seqs : (k + 1) * seqs, :] = (expert * cap + rank == spot).astype(F32).astype(BF16)
        shares[k * seqs : (k + 1) * seqs, :] = jnp.broadcast_to(column(route[k : k + 1]), (seqs, LANES))


def project_kernel(n, *refs):
    ins, weights, outs = refs[:n], refs[n : n + 3], refs[n + 4 :]
    seqs = ins[0].shape[0]
    rows = jnp.concatenate([ref[...] for ref in ins], axis=0)
    for j, weight in enumerate(weights):
        cols = weight.shape[1]
        got = dot(rows, weight[...])
        for k, out in enumerate(outs):
            out[:, j * cols : (j + 1) * cols] = got[k * seqs : (k + 1) * seqs]


def attention_kernel(n, total_heads, lengths, lam, *refs):
    parts = refs[:n]
    head_gain, keys, values, w_out, mine, theirs, fresh_k, fresh_v, spread, scores, fresh_share, *mixed = refs[n:]
    seqs, spots, cols = keys.shape
    width = w_out.shape[1]
    heads = lam.shape[1]
    wide = cols // heads
    head_dim = wide // 2
    maps = 2 * heads
    used = maps * seqs
    per = SUB // maps
    total = parts[0][...]
    for part in parts[1:]:
        total = total + part[...]
    projected = total.astype(BF16)
    query, fresh, value = (projected[:, j * cols : (j + 1) * cols] for j in range(3))
    fresh_k[...] = fresh
    fresh_v[...] = value
    repeat = lax.broadcasted_iota(jnp.int32, (used, seqs), 0) // maps
    repeat = (repeat == lax.broadcasted_iota(jnp.int32, (used, seqs), 1)).astype(F32).astype(BF16)
    row = lax.broadcasted_iota(jnp.int32, (used, cols), 0)
    col = lax.broadcasted_iota(jnp.int32, (used, cols), 1)
    query = jnp.where(row % maps == col // head_dim, dot(repeat, query), 0.0)
    spread[...] = query
    factor = head_dim ** (-0.5)
    new = jnp.sum(query * dot(repeat, fresh), axis=1, keepdims=True) * factor
    inside = lax.broadcasted_iota(jnp.int32, (SUB, 1), 0) // maps

    def one_score(i, carry):
        at = pl.ds(pl.multiple_of(i * SUB, SUB), SUB)
        block, got = spread[at, :], 0.0
        for p in range(per):
            lhs = jnp.where(inside == p, block, 0.0).astype(BF16)
            got += lax.dot_general(lhs, keys[i * per + p], (((1,), (1,)), ((), ())), preferred_element_type=F32)
        scores[at, :] = got
        return carry

    lax.fori_loop(0, used // SUB, one_score, 0, unroll=True)
    line = lax.broadcasted_iota(jnp.int32, (used, LANES), 0)
    whose = line[:, :seqs] // maps == lax.broadcasted_iota(jnp.int32, (used, seqs), 1)
    count = jnp.sum(jnp.where(whose, lengths[...].astype(F32), 0.0), axis=1, keepdims=True)
    head = (lax.axis_index("tp") * heads + (line % maps) // 2).astype(F32)
    slope = jnp.exp2(-8.0 * (head + 1.0) / total_heads)
    mix = jnp.zeros((used, LANES), F32)
    for h in range(heads):
        mix = jnp.where((line % maps) // 2 == h, lam[:, h : h + 1], mix)
    pieces = []
    top = jnp.broadcast_to(new, (used, LANES))
    for at in range(0, spots, LANES):
        spot = (lax.broadcasted_iota(jnp.int32, (used, LANES), 1) + at).astype(F32)
        piece = scores[:, at : at + LANES] * factor - slope * (count - spot)
        piece = jnp.where(spot < count, piece, -jnp.inf)
        pieces.append(piece)
        top = jnp.maximum(top, piece)
    top = jnp.max(top, axis=1, keepdims=True)
    new = jnp.exp(new - top)
    pieces = [jnp.exp(piece - top) for piece in pieces]
    norm = 1.0 / (jnp.sum(functools.reduce(jnp.add, pieces), axis=1, keepdims=True) + new)

    def blend(piece):
        piece = piece * norm
        return piece - mix * pltpu.roll(piece, used - 1, 0)

    for j, piece in enumerate(pieces):
        scores[:, j * LANES : (j + 1) * LANES] = blend(piece)
    fresh_share[...] = blend(jnp.broadcast_to(new, (used, LANES)))

    def one_mix(i, carry):
        at = pl.ds(pl.multiple_of(i * SUB, SUB), SUB)
        block, got = scores[at, :], 0.0
        for p in range(per):
            lhs = jnp.where(inside == p, block, 0.0).astype(BF16)
            got += dot(lhs, values[i * per + p])
        for h in range(heads):
            mixed[h][at, :] = got[:, h * wide : (h + 1) * wide]
        return carry

    lax.fori_loop(0, used // SUB, one_mix, 0, unroll=True)
    outs = []
    for h in range(heads):
        at = slice(h * wide, (h + 1) * wide)
        rows = pl.ds(2 * h, seqs, stride=maps)
        share = fresh_share[rows, :].astype(BF16).astype(F32)
        both = mixed[h][rows, :] + share * value[:, at].astype(F32)
        mean = jnp.mean(both * both, axis=1, keepdims=True)
        outs.append((both * lax.rsqrt(mean + EPS) * head_gain[...]).astype(BF16))
    out = jnp.concatenate(outs, axis=1)
    first = lax.axis_index("tp") % CORES == 0
    slab = width * heads // total_heads
    for z in range(mine.shape[1] // slab):
        at, start = slice(z * slab, (z + 1) * slab), z * CORES * slab
        even, odd = (dot(out, w_out[:, lo : lo + slab]) for lo in (start, start + slab))
        mine[:, at] = jnp.where(first, even, odd).astype(BF16)
        theirs[:, at] = jnp.where(first, odd, even).astype(BF16)


def pair_kernel(mine, got, out):
    out[...] = (mine[...].astype(F32) + got[...].astype(F32)).astype(BF16)


def dispatch_kernel(n_ep, n_tp, n, picker, tokens, *refs):
    parts, resid, outs = refs[:n], refs[n], refs[n + 1 :]
    cap = outs[0].shape[0]
    index = lax.axis_index("tp")
    own = jnp.zeros(resid.shape, F32)
    for z, at, cut in slabs(tokens.shape[1], n_tp, index % CORES):
        total = parts[0][:, at].astype(F32)
        for part in parts[1:]:
            total = total + part[:, at].astype(F32)
        total = tokens[:, cut].astype(F32) + total
        own = jnp.where(index // CORES == z, total, own)
        rows = dot(picker[...], total.astype(BF16)).astype(BF16)
        for k, out in enumerate(outs):
            out[:, at] = rows[k * cap : (k + 1) * cap]
    resid[...] = own


def stack_kernel(*refs):
    for k, ref in enumerate(refs[:-1]):
        cap = ref.shape[0]
        refs[-1][k * cap : (k + 1) * cap, :] = ref[...]


def expert_kernel(n_ep, n_tp, mine, theirs, gain, w_gate, w_up, w_down, back):
    slab = back.shape[2]
    cap = back.shape[1] // n_tp
    width = slab * n_tp
    core = lax.axis_index("tp") % CORES
    blocks = []
    for head, tail, parity in ((mine, theirs, core), (theirs, mine, 1 - core)):
        for _, at, cut in slabs(width, n_tp, parity):
            blocks.append((cut, jnp.concatenate([head[:cap, at].astype(F32), tail[cap:, at].astype(F32)], axis=0)))
    square = sum(jnp.sum(x * x, axis=1, keepdims=True) for _, x in blocks)
    scale = lax.rsqrt(square * (1.0 / width) + EPS)
    gate, upper = 0.0, 0.0
    for cut, x in blocks:
        x = (x * scale * gain[:, cut]).astype(BF16)
        gate += dot(x, w_gate[0, cut, :])
        upper += dot(x, w_up[0, cut, :])
    hidden = (gate * (1.0 / (1.0 + jnp.exp(-gate))) * upper).astype(BF16)
    for t in range(n_tp):
        down = dot(hidden, w_down[0, :, t * slab : (t + 1) * slab]).astype(BF16)
        for k in range(n_ep):
            back[lax.axis_index("ep") ^ k, t * cap : (t + 1) * cap, :] = down[k * cap : (k + 1) * cap]


def combine_kernel(n_ep, n_tp, back, resid, picks, shares, mixed):
    seqs, slab = resid.shape
    cap = back.shape[0] // (n_ep * n_tp)
    outs = []
    for e in range(n_ep):
        total = jnp.zeros((cap, slab), F32)
        for t in range(n_tp):
            lo = (e * n_tp + t) * cap
            total = total + back[lo : lo + cap, :].astype(F32)
        outs.append(total)
    picked = dot(picks[...], jnp.concatenate(outs, axis=0).astype(BF16))
    total = resid[...]
    for k in range(picked.shape[0] // seqs):
        lines = slice(k * seqs, (k + 1) * seqs)
        total = total + shares[lines, :1] * picked[lines]
    mixed[...] = total.astype(BF16)


def on_device(
    n_ep, n_tp,
    tokens, attn_gain, w_query, w_key, w_value, mix_lambda, head_gain, w_output, cache_keys, cache_value, lengths,
    moe_gain, group_ids, member_ids, group_gate, member_logits, w_exp_gate, w_exp_up, w_exp_down,
):
    seqs, width = tokens.shape
    cols = w_query.shape[1]
    slab = width // n_tp
    groups = n_ep * w_exp_gate.shape[0] // EPG
    heads = mix_lambda.shape[0]
    shape = jax.ShapeDtypeStruct

    def send(piece, axis, count, k):
        return lax.ppermute(piece, axis, [(i, i ^ k) for i in range(count)])

    def swap(pieces):
        return [pieces[0]] + [send(piece, "ep", n_ep, k) for k, piece in enumerate(pieces) if k]

    def cross(pieces):
        pairs = itertools.product(range(n_ep), range(n_tp))
        pairs = [(e, t, e * n_tp + t) for e, t in pairs]
        return [pieces[0]] + [
            lax.ppermute(piece, ("ep", "tp"), [(i, (e ^ k) * n_tp + (t ^ 1)) for e, t, i in pairs])
            for k, piece in enumerate(pieces)
            if k
        ]

    slices = pl.pallas_call(
        slices_kernel,
        out_shape=[shape((seqs, width // n_ep), BF16)] * n_ep,
        in_specs=[HBM] * 2,
        out_specs=[VMEM] * n_ep,
        scratch_shapes=[
            pltpu.VMEM((seqs, width), BF16),
            pltpu.VMEM((1, width), F32),
            pltpu.SemaphoreType.DMA((n_ep + 1,)),
        ],
        compiler_params=params(2),
        cost_estimate=cost(2e10),
        name="slices",
    )(*(pltpu.with_memory_space_constraint(x, pltpu.HBM) for x in (tokens, attn_gain.reshape(1, width))))
    pairs = n_ep * n_tp * (seqs // groups)
    top = member_ids.shape[1]
    picker, picks, shares = pl.pallas_call(
        functools.partial(tables_kernel, groups),
        out_shape=[shape((pairs // n_tp, seqs), BF16), shape((top * seqs, pairs // n_tp), BF16), shape((top * seqs, LANES), F32)],
        in_specs=[VMEM] * 4,
        out_specs=[VMEM] * 3,
        compiler_params=params(2),
        cost_estimate=cost(1e9),
        name="tables",
    )(group_ids.reshape(1, seqs), member_ids.T, member_logits.T, group_gate.reshape(1, seqs))
    parts = pl.pallas_call(
        functools.partial(project_kernel, n_ep),
        out_shape=[shape((seqs, 3 * cols), F32)] * n_ep,
        in_specs=[VMEM] * (n_ep + 3) + [ANY],
        out_specs=[VMEM] * n_ep,
        compiler_params=params(6),
        cost_estimate=cost(2e10),
        name="project",
    )(*cross(slices), w_query, w_key, w_value, shares)
    mine, theirs, fresh_keys, fresh_value = pl.pallas_call(
        functools.partial(attention_kernel, n_ep, heads * n_tp),
        out_shape=[shape((seqs, width // CORES), BF16)] * 2 + [shape((seqs, cols), BF16)] * 2,
        in_specs=[VMEM] * (n_ep + 6),
        out_specs=[VMEM] * 4,
        scratch_shapes=[
            pltpu.VMEM((2 * heads * seqs, cols), F32),
            pltpu.VMEM((2 * heads * seqs, cache_keys.shape[1]), F32),
        ]
        + [pltpu.VMEM((2 * heads * seqs, LANES), F32)] * (1 + heads),
        compiler_params=pltpu.CompilerParams(vmem_limit_bytes=6 << 20),
        cost_estimate=cost(1e10),
        name="attention",
    )(
        lengths.reshape(1, seqs), mix_lambda.reshape(1, heads), *swap(parts), head_gain.reshape(1, -1),
        cache_keys, cache_value, w_output,
    )
    pair = pl.pallas_call(
        pair_kernel,
        out_shape=shape(mine.shape, BF16),
        in_specs=[VMEM] * 2,
        out_specs=VMEM,
        compiler_params=params(2),
        cost_estimate=cost(5e8),
        name="pair",
    )(mine, send(theirs, "tp", n_tp, 1))
    halves = [pair] + [send(pair, "tp", n_tp, CORES * k) for k in range(1, n_tp // CORES)]
    cap = seqs // groups
    resid, *rows = pl.pallas_call(
        functools.partial(dispatch_kernel, n_ep, n_tp, len(halves)),
        out_shape=[shape((seqs, slab), F32)] + [shape((cap, width // CORES), BF16)] * n_ep,
        in_specs=[VMEM] * (2 + len(halves)),
        out_specs=[VMEM] * (1 + n_ep),
        compiler_params=params(2),
        cost_estimate=cost(5e9),
        name="dispatch",
    )(picker, tokens, *halves)
    mine = pl.pallas_call(
        stack_kernel,
        out_shape=shape((n_ep * cap, width // CORES), BF16),
        in_specs=[VMEM] * n_ep,
        out_specs=VMEM,
        compiler_params=params(2),
        cost_estimate=cost(5e8),
        name="stack",
    )(*cross(rows))
    back = pl.pallas_call(
        functools.partial(expert_kernel, n_ep, n_tp),
        out_shape=shape((n_ep, n_tp * cap, slab), BF16),
        in_specs=[VMEM] * 6,
        out_specs=VMEM,
        compiler_params=params(10),
        cost_estimate=cost(5e9),
        name="experts",
    )(mine, send(mine, "tp", n_tp, 1), moe_gain.reshape(1, width), w_exp_gate, w_exp_up, w_exp_down)
    back = back.reshape(pairs, slab)
    back = lax.all_to_all(back, ("ep", "tp"), split_axis=0, concat_axis=0, tiled=True)
    mixed = pl.pallas_call(
        functools.partial(combine_kernel, n_ep, n_tp),
        out_shape=shape((seqs, slab), BF16),
        in_specs=[VMEM] * 4,
        out_specs=VMEM,
        compiler_params=params(2),
        cost_estimate=cost(1e9),
        name="combine",
    )(back, resid, picks, shares)
    return mixed, fresh_keys, fresh_value


def solution(mesh):
    return jax.shard_map(
        functools.partial(on_device, mesh.shape["ep"], mesh.shape["tp"]),
        mesh=mesh,
        in_specs=(
            P("ep", None), P(), P("ep", "tp"), P("ep", "tp"), P("ep", "tp"), P("tp"), P(), P("tp", None),
            P("ep", None, "tp"), P("ep", None, "tp"), P("ep"), P(), P("ep"), P("ep", None), P("ep"), P("ep", None),
            P("ep", None, "tp"), P("ep", None, "tp"), P("ep", "tp", None),
        ),
        out_specs=(P("ep", "tp"), P("ep", "tp"), P("ep", "tp")),
        check_vma=False,
    )
```

```python
import functools
import itertools

import jax
import jax.numpy as jnp
from jax import lax
from jax.experimental import pallas as pl
from jax.experimental.pallas import tpu as pltpu
from jax.sharding import PartitionSpec as P

EPG = 2
EPS = 1e-06
F32, BF16 = jnp.float32, jnp.bfloat16
LANES, SUB = 128, 8
CORES = 2
VMEM = pl.BlockSpec(memory_space=pltpu.VMEM)
HBM = pl.BlockSpec(memory_space=pltpu.HBM)
ANY = pl.BlockSpec(memory_space=pl.ANY)


def params(mib):
    return pltpu.CompilerParams(vmem_limit_bytes=mib << 20)


def cost(flops):
    return pl.CostEstimate(flops=int(flops), bytes_accessed=1 << 20, transcendentals=0)


def dot(a, b):
    return jnp.dot(a, b, preferred_element_type=F32)


def slabs(width, n_tp, parity):
    slab = width // n_tp
    for z in range(n_tp // CORES):
        start = (z * CORES + parity) * slab
        yield z, slice(z * slab, (z + 1) * slab), pl.ds(pl.multiple_of(start, LANES), slab)


def slices_kernel(tokens_hbm, gain_hbm, *refs):
    *outs, tokens, gain, sems = refs
    n = len(outs)
    seqs, width = tokens.shape
    cols = width // n
    copies = [pltpu.make_async_copy(gain_hbm, gain, sems.at[n])]
    for k in range(n):
        at = slice(k * cols, (k + 1) * cols)
        copies.append(pltpu.make_async_copy(tokens_hbm.at[:, at], tokens.at[:, at], sems.at[k]))
    for copy in copies:
        copy.start()
    for copy in copies:
        copy.wait()
    x = tokens[...].astype(F32)
    scale = lax.rsqrt(jnp.sum(x * x, axis=1, keepdims=True) * (1.0 / width) + EPS)
    for k, out in enumerate(outs):
        at = pl.ds(pl.multiple_of((lax.axis_index("ep") ^ k) * cols, LANES), cols)
        out[...] = (tokens[:, at].astype(F32) * scale * gain[:, at]).astype(BF16)


def tables_kernel(groups, group_ids, member_ids, logits, gate, picker, picks, shares):
    top, seqs = member_ids.shape
    cap = seqs // groups
    row = lax.broadcasted_iota(jnp.int32, (seqs, seqs), 0)
    col = lax.broadcasted_iota(jnp.int32, (seqs, seqs), 1)

    def column(line):
        return jnp.sum(jnp.where(row == col, line, 0.0), axis=1, keepdims=True)

    group = group_ids[...].astype(F32)
    same = column(group) == group
    rank_line = jnp.sum(jnp.where(same & (row < col), 1.0, 0.0), axis=0, keepdims=True)
    rank = jnp.sum(jnp.where(same & (col < row), 1.0, 0.0), axis=1, keepdims=True)
    spot = lax.broadcasted_iota(jnp.int32, picker.shape, 0)
    wanted = ((lax.axis_index("ep") ^ (spot // cap)) // EPG).astype(F32)
    here = (group == wanted) & (rank_line == (spot % cap).astype(F32))
    picker[...] = here.astype(F32).astype(BF16)
    route = jnp.exp(logits[...] - jnp.max(logits[...], axis=0, keepdims=True))
    route = route / jnp.sum(route, axis=0, keepdims=True) * gate[...]
    spot = lax.broadcasted_iota(jnp.int32, (seqs, picks.shape[1]), 1).astype(F32)
    for k in range(top):
        expert = column(group * EPG + member_ids[k : k + 1, :].astype(F32))
        picks[k * seqs : (k + 1) * seqs, :] = (expert * cap + rank == spot).astype(F32).astype(BF16)
        shares[k * seqs : (k + 1) * seqs, :] = jnp.broadcast_to(column(route[k : k + 1]), (seqs, LANES))


def project_kernel(n, *refs):
    ins, weights, outs = refs[:n], refs[n : n + 3], refs[n + 4 :]
    seqs = ins[0].shape[0]
    rows = jnp.concatenate([ref[...] for ref in ins], axis=0)
    for j, weight in enumerate(weights):
        cols = weight.shape[1]
        got = dot(rows, weight[...])
        for k, out in enumerate(outs):
            out[:, j * cols : (j + 1) * cols] = got[k * seqs : (k + 1) * seqs]


def attention_kernel(n, total_heads, lengths, lam, *refs):
    parts = refs[:n]
    head_gain, keys, values, w_out, mine, theirs, fresh_k, fresh_v, spread, scores, fresh_share, *mixed = refs[n:]
    seqs, spots, cols = keys.shape
    width = w_out.shape[1]
    heads = lam.shape[1]
    wide = cols // heads
    head_dim = wide // 2
    maps = 2 * heads
    used = maps * seqs
    per = SUB // maps
    total = parts[0][...]
    for part in parts[1:]:
        total = total + part[...]
    projected = total.astype(BF16)
    query, fresh, value = (projected[:, j * cols : (j + 1) * cols] for j in range(3))
    fresh_k[...] = fresh
    fresh_v[...] = value
    repeat = lax.broadcasted_iota(jnp.int32, (used, seqs), 0) // maps
    repeat = (repeat == lax.broadcasted_iota(jnp.int32, (used, seqs), 1)).astype(F32).astype(BF16)
    row = lax.broadcasted_iota(jnp.int32, (used, cols), 0)
    col = lax.broadcasted_iota(jnp.int32, (used, cols), 1)
    query = jnp.where(row % maps == col // head_dim, dot(repeat, query), 0.0)
    spread[...] = query
    factor = head_dim ** (-0.5)
    new = jnp.sum(query * dot(repeat, fresh), axis=1, keepdims=True) * factor
    inside = lax.broadcasted_iota(jnp.int32, (SUB, 1), 0) // maps

    def one_score(i, carry):
        at = pl.ds(pl.multiple_of(i * SUB, SUB), SUB)
        block, got = spread[at, :], 0.0
        for p in range(per):
            lhs = jnp.where(inside == p, block, 0.0).astype(BF16)
            got += lax.dot_general(lhs, keys[i * per + p], (((1,), (1,)), ((), ())), preferred_element_type=F32)
        scores[at, :] = got
        return carry

    lax.fori_loop(0, used // SUB, one_score, 0, unroll=True)
    line = lax.broadcasted_iota(jnp.int32, (used, LANES), 0)
    whose = line[:, :seqs] // maps == lax.broadcasted_iota(jnp.int32, (used, seqs), 1)
    count = jnp.sum(jnp.where(whose, lengths[...].astype(F32), 0.0), axis=1, keepdims=True)
    head = (lax.axis_index("tp") * heads + (line % maps) // 2).astype(F32)
    slope = jnp.exp2(-8.0 * (head + 1.0) / total_heads)
    mix = jnp.zeros((used, LANES), F32)
    for h in range(heads):
        mix = jnp.where((line % maps) // 2 == h, lam[:, h : h + 1], mix)
    pieces = []
    top = jnp.broadcast_to(new, (used, LANES))
    for at in range(0, spots, LANES):
        spot = (lax.broadcasted_iota(jnp.int32, (used, LANES), 1) + at).astype(F32)
        piece = scores[:, at : at + LANES] * factor - slope * (count - spot)
        piece = jnp.where(spot < count, piece, -jnp.inf)
        pieces.append(piece)
        top = jnp.maximum(top, piece)
    top = jnp.max(top, axis=1, keepdims=True)
    new = jnp.exp(new - top)
    pieces = [jnp.exp(piece - top) for piece in pieces]
    norm = 1.0 / (jnp.sum(functools.reduce(jnp.add, pieces), axis=1, keepdims=True) + new)

    def blend(piece):
        piece = piece * norm
        return piece - mix * pltpu.roll(piece, used - 1, 0)

    for j, piece in enumerate(pieces):
        scores[:, j * LANES : (j + 1) * LANES] = blend(piece)
    fresh_share[...] = blend(jnp.broadcast_to(new, (used, LANES)))

    def one_mix(i, carry):
        at = pl.ds(pl.multiple_of(i * SUB, SUB), SUB)
        block, got = scores[at, :], 0.0
        for p in range(per):
            lhs = jnp.where(inside == p, block, 0.0).astype(BF16)
            got += dot(lhs, values[i * per + p])
        for h in range(heads):
            mixed[h][at, :] = got[:, h * wide : (h + 1) * wide]
        return carry

    lax.fori_loop(0, used // SUB, one_mix, 0, unroll=True)
    outs = []
    for h in range(heads):
        at = slice(h * wide, (h + 1) * wide)
        rows = pl.ds(2 * h, seqs, stride=maps)
        share = fresh_share[rows, :].astype(BF16).astype(F32)
        both = mixed[h][rows, :] + share * value[:, at].astype(F32)
        mean = jnp.mean(both * both, axis=1, keepdims=True)
        outs.append((both * lax.rsqrt(mean + EPS) * head_gain[...]).astype(BF16))
    out = jnp.concatenate(outs, axis=1)
    first = lax.axis_index("tp") % CORES == 0
    slab = width * heads // total_heads
    for z in range(mine.shape[1] // slab):
        at, start = slice(z * slab, (z + 1) * slab), z * CORES * slab
        even, odd = (dot(out, w_out[:, lo : lo + slab]) for lo in (start, start + slab))
        mine[:, at] = jnp.where(first, even, odd).astype(BF16)
        theirs[:, at] = jnp.where(first, odd, even).astype(BF16)


def pair_kernel(mine, got, out):
    out[...] = (mine[...].astype(F32) + got[...].astype(F32)).astype(BF16)


def dispatch_kernel(n_ep, n_tp, n, picker, tokens, *refs):
    parts, resid, outs = refs[:n], refs[n], refs[n + 1 :]
    cap = outs[0].shape[0]
    index = lax.axis_index("tp")
    own = jnp.zeros(resid.shape, F32)
    for z, at, cut in slabs(tokens.shape[1], n_tp, index % CORES):
        total = parts[0][:, at].astype(F32)
        for part in parts[1:]:
            total = total + part[:, at].astype(F32)
        total = tokens[:, cut].astype(F32) + total
        own = jnp.where(index // CORES == z, total, own)
        rows = dot(picker[...], total.astype(BF16)).astype(BF16)
        for k, out in enumerate(outs):
            out[:, at] = rows[k * cap : (k + 1) * cap]
    resid[...] = own


def stack_kernel(*refs):
    for k, ref in enumerate(refs[:-1]):
        cap = ref.shape[0]
        refs[-1][k * cap : (k + 1) * cap, :] = ref[...]


def expert_kernel(n_ep, n_tp, mine, theirs, gain, w_gate, w_up, w_down, back):
    slab = back.shape[2]
    cap = back.shape[1] // n_tp
    width = slab * n_tp
    core = lax.axis_index("tp") % CORES
    blocks = []
    for head, tail, parity in ((mine, theirs, core), (theirs, mine, 1 - core)):
        for _, at, cut in slabs(width, n_tp, parity):
            blocks.append((cut, jnp.concatenate([head[:cap, at].astype(F32), tail[cap:, at].astype(F32)], axis=0)))
    square = sum(jnp.sum(x * x, axis=1, keepdims=True) for _, x in blocks)
    scale = lax.rsqrt(square * (1.0 / width) + EPS)
    gate, upper = 0.0, 0.0
    for cut, x in blocks:
        x = (x * scale * gain[:, cut]).astype(BF16)
        gate += dot(x, w_gate[0, cut, :])
        upper += dot(x, w_up[0, cut, :])
    hidden = (gate * (1.0 / (1.0 + jnp.exp(-gate))) * upper).astype(BF16)
    for t in range(n_tp):
        down = dot(hidden, w_down[0, :, t * slab : (t + 1) * slab]).astype(BF16)
        for k in range(n_ep):
            back[lax.axis_index("ep") ^ k, t * cap : (t + 1) * cap, :] = down[k * cap : (k + 1) * cap]


def combine_kernel(n_ep, n_tp, back, resid, picks, shares, mixed):
    seqs, slab = resid.shape
    cap = back.shape[0] // (n_ep * n_tp)
    outs = []
    for e in range(n_ep):
        total = jnp.zeros((cap, slab), F32)
        for t in range(n_tp):
            lo = (e * n_tp + t) * cap
            total = total + back[lo : lo + cap, :].astype(F32)
        outs.append(total)
    picked = dot(picks[...], jnp.concatenate(outs, axis=0).astype(BF16))
    total = resid[...]
    for k in range(picked.shape[0] // seqs):
        lines = slice(k * seqs, (k + 1) * seqs)
        total = total + shares[lines, :1] * picked[lines]
    mixed[...] = total.astype(BF16)


def on_device(
    n_ep, n_tp,
    tokens, attn_gain, w_query, w_key, w_value, mix_lambda, head_gain, w_output, cache_keys, cache_value, lengths,
    moe_gain, group_ids, member_ids, group_gate, member_logits, w_exp_gate, w_exp_up, w_exp_down,
):
    seqs, width = tokens.shape
    cols = w_query.shape[1]
    slab, n_z = width // n_tp, n_tp // CORES
    groups = n_ep * w_exp_gate.shape[0] // EPG
    heads = mix_lambda.shape[0]
    shape = jax.ShapeDtypeStruct

    def send(piece, axis, count, k):
        return lax.ppermute(piece, axis, [(i, i ^ k) for i in range(count)])

    def swap(pieces):
        return [pieces[0]] + [send(piece, "ep", n_ep, k) for k, piece in enumerate(pieces) if k]

    def cross(pieces):
        pairs = itertools.product(range(n_ep), range(n_tp))
        pairs = [(e, t, e * n_tp + t) for e, t in pairs]
        return [pieces[0]] + [
            lax.ppermute(piece, ("ep", "tp"), [(i, (e ^ k) * n_tp + (t ^ 1)) for e, t, i in pairs])
            for k, piece in enumerate(pieces)
            if k
        ]

    slices = pl.pallas_call(
        slices_kernel,
        out_shape=[shape((seqs, width // n_ep), BF16)] * n_ep,
        in_specs=[HBM] * 2,
        out_specs=[VMEM] * n_ep,
        scratch_shapes=[
            pltpu.VMEM((seqs, width), BF16),
            pltpu.VMEM((1, width), F32),
            pltpu.SemaphoreType.DMA((n_ep + 1,)),
        ],
        compiler_params=params(2),
        cost_estimate=cost(2e10),
        name="slices",
    )(*(pltpu.with_memory_space_constraint(x, pltpu.HBM) for x in (tokens, attn_gain.reshape(1, width))))
    pairs = n_ep * n_tp * (seqs // groups)
    top = member_ids.shape[1]
    picker, picks, shares = pl.pallas_call(
        functools.partial(tables_kernel, groups),
        out_shape=[shape((pairs // n_tp, seqs), BF16), shape((top * seqs, pairs // n_tp), BF16), shape((top * seqs, LANES), F32)],
        in_specs=[VMEM] * 4,
        out_specs=[VMEM] * 3,
        compiler_params=params(2),
        cost_estimate=cost(1e9),
        name="tables",
    )(group_ids.reshape(1, seqs), member_ids.T, member_logits.T, group_gate.reshape(1, seqs))
    parts = pl.pallas_call(
        functools.partial(project_kernel, n_ep),
        out_shape=[shape((seqs, 3 * cols), F32)] * n_ep,
        in_specs=[VMEM] * (n_ep + 3) + [ANY],
        out_specs=[VMEM] * n_ep,
        compiler_params=params(6),
        cost_estimate=cost(2e10),
        name="project",
    )(*cross(slices), w_query, w_key, w_value, shares)
    mine, theirs, fresh_keys, fresh_value = pl.pallas_call(
        functools.partial(attention_kernel, n_ep, heads * n_tp),
        out_shape=[shape((seqs, width // CORES), BF16)] * 2 + [shape((seqs, cols), BF16)] * 2,
        in_specs=[VMEM] * (n_ep + 6),
        out_specs=[VMEM] * 4,
        scratch_shapes=[
            pltpu.VMEM((2 * heads * seqs, cols), F32),
            pltpu.VMEM((2 * heads * seqs, cache_keys.shape[1]), F32),
        ]
        + [pltpu.VMEM((2 * heads * seqs, LANES), F32)] * (1 + heads),
        compiler_params=pltpu.CompilerParams(vmem_limit_bytes=6 << 20),
        cost_estimate=cost(1e10),
        name="attention",
    )(
        lengths.reshape(1, seqs), mix_lambda.reshape(1, heads), *swap(parts), head_gain.reshape(1, -1),
        cache_keys, cache_value, w_output,
    )
    pair = pl.pallas_call(
        pair_kernel,
        out_shape=shape(mine.shape, BF16),
        in_specs=[VMEM] * 2,
        out_specs=VMEM,
        compiler_params=params(2),
        cost_estimate=cost(5e8),
        name="pair",
    )(mine, send(theirs, "tp", n_tp, 1))
    order = list(range(2, n_z))
    order.insert(1, 1)
    halves = [pair] + [send(pair, "tp", n_tp, CORES * k) for k in order]
    cap = seqs // groups
    resid, *rows = pl.pallas_call(
        functools.partial(dispatch_kernel, n_ep, n_tp, len(halves)),
        out_shape=[shape((seqs, slab), F32)] + [shape((cap, width // CORES), BF16)] * n_ep,
        in_specs=[VMEM] * (2 + len(halves)),
        out_specs=[VMEM] * (1 + n_ep),
        compiler_params=params(2),
        cost_estimate=cost(5e9),
        name="dispatch",
    )(picker, tokens, *halves)
    mine = pl.pallas_call(
        stack_kernel,
        out_shape=shape((n_ep * cap, width // CORES), BF16),
        in_specs=[VMEM] * n_ep,
        out_specs=VMEM,
        compiler_params=params(2),
        cost_estimate=cost(5e8),
        name="stack",
    )(*cross(rows))
    back = pl.pallas_call(
        functools.partial(expert_kernel, n_ep, n_tp),
        out_shape=shape((n_ep, n_tp * cap, slab), BF16),
        in_specs=[VMEM] * 6,
        out_specs=VMEM,
        compiler_params=params(10),
        cost_estimate=cost(5e9),
        name="experts",
    )(mine, send(mine, "tp", n_tp, 1), moe_gain.reshape(1, width), w_exp_gate, w_exp_up, w_exp_down)
    back = back.reshape(pairs, slab)
    back = lax.all_to_all(back, ("ep", "tp"), split_axis=0, concat_axis=0, tiled=True)
    mixed = pl.pallas_call(
        functools.partial(combine_kernel, n_ep, n_tp),
        out_shape=shape((seqs, slab), BF16),
        in_specs=[VMEM] * 4,
        out_specs=VMEM,
        compiler_params=params(2),
        cost_estimate=cost(1e9),
        name="combine",
    )(back, resid, picks, shares)
    return mixed, fresh_keys, fresh_value


def solution(mesh):
    return jax.shard_map(
        functools.partial(on_device, mesh.shape["ep"], mesh.shape["tp"]),
        mesh=mesh,
        in_specs=(
            P("ep", None), P(), P("ep", "tp"), P("ep", "tp"), P("ep", "tp"), P("tp"), P(), P("tp", None),
            P("ep", None, "tp"), P("ep", None, "tp"), P("ep"), P(), P("ep"), P("ep", None), P("ep"), P("ep", None),
            P("ep", None, "tp"), P("ep", None, "tp"), P("ep", "tp", None),
        ),
        out_specs=(P("ep", "tp"), P("ep", "tp"), P("ep", "tp")),
        check_vma=False,
    )
```

```python
import functools
import itertools

import jax
import jax.numpy as jnp
from jax import lax
from jax.experimental import pallas as pl
from jax.experimental.pallas import tpu as pltpu
from jax.sharding import PartitionSpec as P

EPG = 2
EPS = 1e-06
F32, BF16 = jnp.float32, jnp.bfloat16
LANES, SUB = 128, 8
CORES = 2
VMEM = pl.BlockSpec(memory_space=pltpu.VMEM)
HBM = pl.BlockSpec(memory_space=pltpu.HBM)
ANY = pl.BlockSpec(memory_space=pl.ANY)


def params(mib):
    return pltpu.CompilerParams(vmem_limit_bytes=mib << 20)


def cost(flops):
    return pl.CostEstimate(flops=int(flops), bytes_accessed=1 << 20, transcendentals=0)


def dot(a, b):
    return jnp.dot(a, b, preferred_element_type=F32)


def slabs(width, n_tp, parity):
    slab = width // n_tp
    for z in range(n_tp // CORES):
        start = (z * CORES + parity) * slab
        yield z, slice(z * slab, (z + 1) * slab), pl.ds(pl.multiple_of(start, LANES), slab)


def slices_kernel(tokens_hbm, gain_hbm, *refs):
    *outs, tokens, gain, sems = refs
    n = len(outs)
    seqs, width = tokens.shape
    cols = width // n
    copies = [pltpu.make_async_copy(gain_hbm, gain, sems.at[n])]
    for k in range(n):
        at = slice(k * cols, (k + 1) * cols)
        copies.append(pltpu.make_async_copy(tokens_hbm.at[:, at], tokens.at[:, at], sems.at[k]))
    for copy in copies:
        copy.start()
    for copy in copies:
        copy.wait()
    x = tokens[...].astype(F32)
    scale = lax.rsqrt(jnp.sum(x * x, axis=1, keepdims=True) * (1.0 / width) + EPS)
    for k, out in enumerate(outs):
        at = pl.ds(pl.multiple_of((lax.axis_index("ep") ^ k) * cols, LANES), cols)
        out[...] = (tokens[:, at].astype(F32) * scale * gain[:, at]).astype(BF16)


def tables_kernel(groups, group_ids, member_ids, logits, gate, picker, picks, shares):
    top, seqs = member_ids.shape
    cap = seqs // groups
    row = lax.broadcasted_iota(jnp.int32, (seqs, seqs), 0)
    col = lax.broadcasted_iota(jnp.int32, (seqs, seqs), 1)

    def column(line):
        return jnp.sum(jnp.where(row == col, line, 0.0), axis=1, keepdims=True)

    group = group_ids[...].astype(F32)
    same = column(group) == group
    rank_line = jnp.sum(jnp.where(same & (row < col), 1.0, 0.0), axis=0, keepdims=True)
    rank = jnp.sum(jnp.where(same & (col < row), 1.0, 0.0), axis=1, keepdims=True)
    spot = lax.broadcasted_iota(jnp.int32, picker.shape, 0)
    wanted = ((lax.axis_index("ep") ^ (spot // cap)) // EPG).astype(F32)
    here = (group == wanted) & (rank_line == (spot % cap).astype(F32))
    picker[...] = here.astype(F32).astype(BF16)
    route = jnp.exp(logits[...] - jnp.max(logits[...], axis=0, keepdims=True))
    route = route / jnp.sum(route, axis=0, keepdims=True) * gate[...]
    spot = lax.broadcasted_iota(jnp.int32, (seqs, picks.shape[1]), 1).astype(F32)
    for k in range(top):
        expert = column(group * EPG + member_ids[k : k + 1, :].astype(F32))
        picks[k * seqs : (k + 1) * seqs, :] = (expert * cap + rank == spot).astype(F32).astype(BF16)
        shares[k * seqs : (k + 1) * seqs, :] = jnp.broadcast_to(column(route[k : k + 1]), (seqs, LANES))


def project_kernel(n, *refs):
    ins, weights, outs = refs[:n], refs[n : n + 3], refs[n + 4 :]
    seqs = ins[0].shape[0]
    rows = jnp.concatenate([ref[...] for ref in ins], axis=0)
    for j, weight in enumerate(weights):
        cols = weight.shape[1]
        got = dot(rows, weight[...])
        for k, out in enumerate(outs):
            out[:, j * cols : (j + 1) * cols] = got[k * seqs : (k + 1) * seqs]


def attention_kernel(n, total_heads, lengths, lam, *refs):
    parts = refs[:n]
    head_gain, keys, values, w_out, mine, theirs, fresh_k, fresh_v, spread, scores, fresh_share, *mixed = refs[n:]
    seqs, spots, cols = keys.shape
    width = w_out.shape[1]
    heads = lam.shape[1]
    wide = cols // heads
    head_dim = wide // 2
    maps = 2 * heads
    used = maps * seqs
    per = SUB // maps
    total = parts[0][...]
    for part in parts[1:]:
        total = total + part[...]
    projected = total.astype(BF16)
    query, fresh, value = (projected[:, j * cols : (j + 1) * cols] for j in range(3))
    fresh_k[...] = fresh
    fresh_v[...] = value
    repeat = lax.broadcasted_iota(jnp.int32, (used, seqs), 0) // maps
    repeat = (repeat == lax.broadcasted_iota(jnp.int32, (used, seqs), 1)).astype(F32).astype(BF16)
    row = lax.broadcasted_iota(jnp.int32, (used, cols), 0)
    col = lax.broadcasted_iota(jnp.int32, (used, cols), 1)
    query = jnp.where(row % maps == col // head_dim, dot(repeat, query), 0.0)
    spread[...] = query
    factor = head_dim ** (-0.5)
    new = jnp.sum(query * dot(repeat, fresh), axis=1, keepdims=True) * factor
    inside = lax.broadcasted_iota(jnp.int32, (SUB, 1), 0) // maps

    def one_score(i, carry):
        at = pl.ds(pl.multiple_of(i * SUB, SUB), SUB)
        block, got = spread[at, :], 0.0
        for p in range(per):
            lhs = jnp.where(inside == p, block, 0.0).astype(BF16)
            got += lax.dot_general(lhs, keys[i * per + p], (((1,), (1,)), ((), ())), preferred_element_type=F32)
        scores[at, :] = got
        return carry

    lax.fori_loop(0, used // SUB, one_score, 0, unroll=True)
    line = lax.broadcasted_iota(jnp.int32, (used, LANES), 0)
    whose = line[:, :seqs] // maps == lax.broadcasted_iota(jnp.int32, (used, seqs), 1)
    count = jnp.sum(jnp.where(whose, lengths[...].astype(F32), 0.0), axis=1, keepdims=True)
    head = (lax.axis_index("tp") * heads + (line % maps) // 2).astype(F32)
    slope = jnp.exp2(-8.0 * (head + 1.0) / total_heads)
    mix = jnp.zeros((used, LANES), F32)
    for h in range(heads):
        mix = jnp.where((line % maps) // 2 == h, lam[:, h : h + 1], mix)
    pieces = []
    top = jnp.broadcast_to(new, (used, LANES))
    for at in range(0, spots, LANES):
        spot = (lax.broadcasted_iota(jnp.int32, (used, LANES), 1) + at).astype(F32)
        piece = scores[:, at : at + LANES] * factor - slope * (count - spot)
        piece = jnp.where(spot < count, piece, -jnp.inf)
        pieces.append(piece)
        top = jnp.maximum(top, piece)
    top = jnp.max(top, axis=1, keepdims=True)
    new = jnp.exp(new - top)
    pieces = [jnp.exp(piece - top) for piece in pieces]
    norm = 1.0 / (jnp.sum(functools.reduce(jnp.add, pieces), axis=1, keepdims=True) + new)

    def blend(piece):
        piece = piece * norm
        return piece - mix * pltpu.roll(piece, used - 1, 0)

    for j, piece in enumerate(pieces):
        scores[:, j * LANES : (j + 1) * LANES] = blend(piece)
    fresh_share[...] = blend(jnp.broadcast_to(new, (used, LANES)))

    def one_mix(i, carry):
        at = pl.ds(pl.multiple_of(i * SUB, SUB), SUB)
        block, got = scores[at, :], 0.0
        for p in range(per):
            lhs = jnp.where(inside == p, block, 0.0).astype(BF16)
            got += dot(lhs, values[i * per + p])
        for h in range(heads):
            mixed[h][at, :] = got[:, h * wide : (h + 1) * wide]
        return carry

    lax.fori_loop(0, used // SUB, one_mix, 0, unroll=True)
    outs = []
    for h in range(heads):
        at = slice(h * wide, (h + 1) * wide)
        rows = pl.ds(2 * h, seqs, stride=maps)
        share = fresh_share[rows, :].astype(BF16).astype(F32)
        both = mixed[h][rows, :] + share * value[:, at].astype(F32)
        mean = jnp.mean(both * both, axis=1, keepdims=True)
        outs.append((both * lax.rsqrt(mean + EPS) * head_gain[...]).astype(BF16))
    out = jnp.concatenate(outs, axis=1)
    first = lax.axis_index("tp") % CORES == 0
    slab = width * heads // total_heads
    for z in range(mine.shape[1] // slab):
        at, start = slice(z * slab, (z + 1) * slab), z * CORES * slab
        even, odd = (dot(out, w_out[:, lo : lo + slab]) for lo in (start, start + slab))
        mine[:, at] = jnp.where(first, even, odd).astype(BF16)
        theirs[:, at] = jnp.where(first, odd, even).astype(BF16)


def pair_kernel(mine, got, out):
    out[...] = (mine[...].astype(F32) + got[...].astype(F32)).astype(BF16)


def dispatch_kernel(n_ep, n_tp, n, picker, tokens, *refs):
    parts, resid, outs = refs[:n], refs[n], refs[n + 1 :]
    cap = outs[0].shape[0]
    index = lax.axis_index("tp")
    own = jnp.zeros(resid.shape, F32)
    for z, at, cut in slabs(tokens.shape[1], n_tp, index % CORES):
        total = parts[0][:, at].astype(F32)
        for part in parts[1:]:
            total = total + part[:, at].astype(F32)
        total = tokens[:, cut].astype(F32) + total
        own = jnp.where(index // CORES == z, total, own)
        rows = dot(picker[...], total.astype(BF16)).astype(BF16)
        for k, out in enumerate(outs):
            out[:, at] = rows[k * cap : (k + 1) * cap]
    resid[...] = own


def stack_kernel(*refs):
    for k, ref in enumerate(refs[:-1]):
        cap = ref.shape[0]
        refs[-1][k * cap : (k + 1) * cap, :] = ref[...]


def expert_kernel(n_ep, n_tp, mine, theirs, gain, w_gate, w_up, w_down, back):
    slab = back.shape[2]
    cap = back.shape[1] // n_tp
    width = slab * n_tp
    core = lax.axis_index("tp") % CORES
    blocks = []
    for head, tail, parity in ((mine, theirs, core), (theirs, mine, 1 - core)):
        for _, at, cut in slabs(width, n_tp, parity):
            blocks.append((cut, jnp.concatenate([head[:cap, at].astype(F32), tail[cap:, at].astype(F32)], axis=0)))
    square = sum(jnp.sum(x * x, axis=1, keepdims=True) for _, x in blocks)
    scale = lax.rsqrt(square * (1.0 / width) + EPS)
    gate, upper = 0.0, 0.0
    for cut, x in blocks:
        x = (x * gain[:, cut]).astype(BF16)
        gate += dot(x, w_gate[0, cut, :])
        upper += dot(x, w_up[0, cut, :])
    gate, upper = gate * scale, upper * scale
    hidden = (gate * (1.0 / (1.0 + jnp.exp(-gate))) * upper).astype(BF16)
    for t in range(n_tp):
        down = dot(hidden, w_down[0, :, t * slab : (t + 1) * slab]).astype(BF16)
        for k in range(n_ep):
            back[lax.axis_index("ep") ^ k, t * cap : (t + 1) * cap, :] = down[k * cap : (k + 1) * cap]


def combine_kernel(n_ep, n_tp, back, resid, picks, shares, mixed):
    seqs, slab = resid.shape
    cap = back.shape[0] // (n_ep * n_tp)
    outs = []
    for e in range(n_ep):
        total = jnp.zeros((cap, slab), F32)
        for t in range(n_tp):
            lo = (e * n_tp + t) * cap
            total = total + back[lo : lo + cap, :].astype(F32)
        outs.append(total)
    picked = dot(picks[...], jnp.concatenate(outs, axis=0).astype(BF16))
    total = resid[...]
    for k in range(picked.shape[0] // seqs):
        lines = slice(k * seqs, (k + 1) * seqs)
        total = total + shares[lines, :1] * picked[lines]
    mixed[...] = total.astype(BF16)


def on_device(
    n_ep, n_tp,
    tokens, attn_gain, w_query, w_key, w_value, mix_lambda, head_gain, w_output, cache_keys, cache_value, lengths,
    moe_gain, group_ids, member_ids, group_gate, member_logits, w_exp_gate, w_exp_up, w_exp_down,
):
    seqs, width = tokens.shape
    cols = w_query.shape[1]
    slab, n_z = width // n_tp, n_tp // CORES
    groups = n_ep * w_exp_gate.shape[0] // EPG
    heads = mix_lambda.shape[0]
    shape = jax.ShapeDtypeStruct

    def send(piece, axis, count, k):
        return lax.ppermute(piece, axis, [(i, i ^ k) for i in range(count)])

    def swap(pieces):
        return [pieces[0]] + [send(piece, "ep", n_ep, k) for k, piece in enumerate(pieces) if k]

    def cross(pieces):
        pairs = itertools.product(range(n_ep), range(n_tp))
        pairs = [(e, t, e * n_tp + t) for e, t in pairs]
        return [pieces[0]] + [
            lax.ppermute(piece, ("ep", "tp"), [(i, (e ^ k) * n_tp + (t ^ 1)) for e, t, i in pairs])
            for k, piece in enumerate(pieces)
            if k
        ]

    slices = pl.pallas_call(
        slices_kernel,
        out_shape=[shape((seqs, width // n_ep), BF16)] * n_ep,
        in_specs=[HBM] * 2,
        out_specs=[VMEM] * n_ep,
        scratch_shapes=[
            pltpu.VMEM((seqs, width), BF16),
            pltpu.VMEM((1, width), F32),
            pltpu.SemaphoreType.DMA((n_ep + 1,)),
        ],
        compiler_params=params(2),
        cost_estimate=cost(2e10),
        name="slices",
    )(*(pltpu.with_memory_space_constraint(x, pltpu.HBM) for x in (tokens, attn_gain.reshape(1, width))))
    pairs = n_ep * n_tp * (seqs // groups)
    top = member_ids.shape[1]
    picker, picks, shares = pl.pallas_call(
        functools.partial(tables_kernel, groups),
        out_shape=[shape((pairs // n_tp, seqs), BF16), shape((top * seqs, pairs // n_tp), BF16), shape((top * seqs, LANES), F32)],
        in_specs=[VMEM] * 4,
        out_specs=[VMEM] * 3,
        compiler_params=params(2),
        cost_estimate=cost(1e9),
        name="tables",
    )(group_ids.reshape(1, seqs), member_ids.T, member_logits.T, group_gate.reshape(1, seqs))
    parts = pl.pallas_call(
        functools.partial(project_kernel, n_ep),
        out_shape=[shape((seqs, 3 * cols), F32)] * n_ep,
        in_specs=[VMEM] * (n_ep + 3) + [ANY],
        out_specs=[VMEM] * n_ep,
        compiler_params=params(6),
        cost_estimate=cost(2e10),
        name="project",
    )(*cross(slices), w_query, w_key, w_value, shares)
    mine, theirs, fresh_keys, fresh_value = pl.pallas_call(
        functools.partial(attention_kernel, n_ep, heads * n_tp),
        out_shape=[shape((seqs, width // CORES), BF16)] * 2 + [shape((seqs, cols), BF16)] * 2,
        in_specs=[VMEM] * (n_ep + 6),
        out_specs=[VMEM] * 4,
        scratch_shapes=[
            pltpu.VMEM((2 * heads * seqs, cols), F32),
            pltpu.VMEM((2 * heads * seqs, cache_keys.shape[1]), F32),
        ]
        + [pltpu.VMEM((2 * heads * seqs, LANES), F32)] * (1 + heads),
        compiler_params=pltpu.CompilerParams(vmem_limit_bytes=6 << 20),
        cost_estimate=cost(1e10),
        name="attention",
    )(
        lengths.reshape(1, seqs), mix_lambda.reshape(1, heads), *swap(parts), head_gain.reshape(1, -1),
        cache_keys, cache_value, w_output,
    )
    pair = pl.pallas_call(
        pair_kernel,
        out_shape=shape(mine.shape, BF16),
        in_specs=[VMEM] * 2,
        out_specs=VMEM,
        compiler_params=params(2),
        cost_estimate=cost(5e8),
        name="pair",
    )(mine, send(theirs, "tp", n_tp, 1))
    order = list(range(2, n_z))
    order.insert(1, 1)
    halves = [pair] + [send(pair, "tp", n_tp, CORES * k) for k in order]
    cap = seqs // groups
    resid, *rows = pl.pallas_call(
        functools.partial(dispatch_kernel, n_ep, n_tp, len(halves)),
        out_shape=[shape((seqs, slab), F32)] + [shape((cap, width // CORES), BF16)] * n_ep,
        in_specs=[VMEM] * (2 + len(halves)),
        out_specs=[VMEM] * (1 + n_ep),
        compiler_params=params(2),
        cost_estimate=cost(5e9),
        name="dispatch",
    )(picker, tokens, *halves)
    mine = pl.pallas_call(
        stack_kernel,
        out_shape=shape((n_ep * cap, width // CORES), BF16),
        in_specs=[VMEM] * n_ep,
        out_specs=VMEM,
        compiler_params=params(2),
        cost_estimate=cost(5e8),
        name="stack",
    )(*cross(rows))
    back = pl.pallas_call(
        functools.partial(expert_kernel, n_ep, n_tp),
        out_shape=shape((n_ep, n_tp * cap, slab), BF16),
        in_specs=[VMEM] * 6,
        out_specs=VMEM,
        compiler_params=params(10),
        cost_estimate=cost(5e9),
        name="experts",
    )(mine, send(mine, "tp", n_tp, 1), moe_gain.reshape(1, width), w_exp_gate, w_exp_up, w_exp_down)
    back = back.reshape(pairs, slab)
    back = lax.all_to_all(back, ("ep", "tp"), split_axis=0, concat_axis=0, tiled=True)
    mixed = pl.pallas_call(
        functools.partial(combine_kernel, n_ep, n_tp),
        out_shape=shape((seqs, slab), BF16),
        in_specs=[VMEM] * 4,
        out_specs=VMEM,
        compiler_params=params(2),
        cost_estimate=cost(1e9),
        name="combine",
    )(back, resid, picks, shares)
    return mixed, fresh_keys, fresh_value


def solution(mesh):
    return jax.shard_map(
        functools.partial(on_device, mesh.shape["ep"], mesh.shape["tp"]),
        mesh=mesh,
        in_specs=(
            P("ep", None), P(), P("ep", "tp"), P("ep", "tp"), P("ep", "tp"), P("tp"), P(), P("tp", None),
            P("ep", None, "tp"), P("ep", None, "tp"), P("ep"), P(), P("ep"), P("ep", None), P("ep"), P("ep", None),
            P("ep", None, "tp"), P("ep", None, "tp"), P("ep", "tp", None),
        ),
        out_specs=(P("ep", "tp"), P("ep", "tp"), P("ep", "tp")),
        check_vma=False,
    )
```
